128 devices in a mesh: sp: 32 (over z, y, core), tp: 4 (over x).
Axes of the slice: x: 4, y: 4, z: 4, core: 2. Of those that a mesh axis runs over, the one named last changes fastest.
Arguments:
- d_out: bfloat16 [16384, 2048], P('sp'), may hold values from -6 to 6
- route_expert: int32 [16384, 2], P('sp'), may hold values from 0 to 31, all different within a row; in each aligned block of 512 rows (0 to 511, 512 to 1023, ...) at most 36 rows name the same one
- route_weight: float32 [16384, 2], P('sp'), may hold values from 0.2 to 1
- expert_inputs: bfloat16 [32, 1152, 2048], P('sp'), may hold values from -6 to 6
- w_gate: bfloat16 [32, 2048, 2816], P('sp', None, 'tp'), may hold values from -0.125 to 0.125
- w_up: bfloat16 [32, 2048, 2816], P('sp', None, 'tp'), may hold values from -0.125 to 0.125
- w_down: bfloat16 [32, 2816, 2048], P('sp', 'tp'), may hold values from -0.109375 to 0.109375
- w_out: bfloat16 [2048, 1024], P(None, 'tp'), may hold values from -0.1875 to 0.1875
- queries: bfloat16 [16384, 4, 128], P('sp', 'tp'), may hold values from -6 to 6
- keys: bfloat16 [16384, 4, 128], P('sp', 'tp'), may hold values from -1.25 to 1.25
- values: bfloat16 [16384, 4, 256], P('sp', 'tp'), may hold values from -6 to 6
- log_decay: float32 [16384, 4, 128], P('sp', 'tp'), may hold values from -1 to 0
Outputs:
- grad_gate: bfloat16 [32, 2048, 2816], P('sp', None, 'tp')
- grad_up: bfloat16 [32, 2048, 2816], P('sp', None, 'tp')
- grad_down: bfloat16 [32, 2816, 2048], P('sp', 'tp')
- grad_proj: float32 [2048, 1024], P('sp', 'tp')
- grad_queries: bfloat16 [16384, 4, 128], P('sp', 'tp')
- grad_keys: bfloat16 [16384, 4, 128], P('sp', 'tp')
- grad_values: bfloat16 [16384, 4, 256], P('sp', 'tp')
- grad_log_decay: float32 [16384, 4, 128], P('sp', 'tp')
The draws below stay inside these ranges and needn't reach their ends.
Inputs may be any that keep to these rules, and one draw needn't show every extreme that they name: `route_expert`: the two experts of a token differ. Among the rows of one device no expert is named more than 36 times, and in every draw some device names some expert exactly 36 times.
All inputs are finite; a program needn't handle non-finite values.
Results may differ from the reference program's by a relative error of at most 0.02.
Values may be sent and summed in bfloat16 or wider, within the bound.
A program may use at most 128 MiB of HBM per device.

```python
import math
import jax
import jax.numpy as jnp
import numpy as np
from jax import lax

D = 2048
FF = 2816
MIXER_HEADS = 4
KEY_CHANNELS = 128
DV = 256
BLK = 64
TOK_DEV = 512
SEQUENCE_TOKENS = 16384
EXPERTS = 32
CAP = 36
N_SP = 32
N_TP = 4


def draw_log_decay(key, part):
    every_head_keys = jax.random.split(jax.random.fold_in(key, 11), 7)
    slow_share = 0.5
    gradual_decay_mask = jax.random.bernoulli(every_head_keys[0], slow_share, (MIXER_HEADS, KEY_CHANNELS))
    slow_rate = jnp.exp(jax.random.uniform(every_head_keys[1], (MIXER_HEADS, KEY_CHANNELS), jnp.float32, jnp.log(0.05), jnp.log(0.5))) / SEQUENCE_TOKENS
    fast_rate = jnp.exp(jax.random.uniform(every_head_keys[2], (MIXER_HEADS, KEY_CHANNELS), jnp.float32, jnp.log(0.01), jnp.log(0.033)))
    base_rate = jnp.where(gradual_decay_mask, slow_rate, fast_rate)
    segment_count = SEQUENCE_TOKENS // TOK_DEV
    device_factor = jnp.exp(jax.random.uniform(every_head_keys[3], (segment_count, 1, 1, 1), jnp.float32, jnp.log(0.5), jnp.log(2.0)))
    device_factor = jnp.broadcast_to(device_factor, (segment_count, TOK_DEV, 1, 1)).reshape(SEQUENCE_TOKENS, 1, 1)
    roughness = jax.random.uniform(every_head_keys[4], (SEQUENCE_TOKENS, MIXER_HEADS, KEY_CHANNELS), jnp.float32, 0.5, 1.5)
    spike_position = jax.random.randint(every_head_keys[5], (4,), 0, SEQUENCE_TOKENS)
    spike_token_rows = jnp.any(jnp.arange(SEQUENCE_TOKENS)[:, None] == spike_position[None, :], axis=1)
    spike_penalty = jnp.log(jax.random.uniform(every_head_keys[6], (SEQUENCE_TOKENS, MIXER_HEADS, KEY_CHANNELS), jnp.float32, 0.5, 0.8))
    channel_decay_logs = -base_rate[None] * device_factor * roughness
    channel_decay_logs = channel_decay_logs + jnp.where(spike_token_rows[:, None, None] & gradual_decay_mask[None], spike_penalty, 0.0)
    return channel_decay_logs.astype(jnp.float32)


def with_spikes(drawn, own_key, source, target, shards_of, factor):
    def block_of(position):
        return (jnp.arange(drawn.shape[position]) // (drawn.shape[position] // shards_of)).reshape((-1,) + (1,) * (drawn.ndim - 1 - position))

    near = jax.random.permutation(own_key, shards_of)[block_of(target)]
    far = (block_of(target) + shards_of // 2) % shards_of
    return jnp.where((block_of(source) == near) | (block_of(source) == far), factor * drawn, drawn)


def levels(rng, dims, shards, least, largest):
    loudness = 1.0
    for dim, shards_of in shards:
        steps = jax.random.uniform(jax.random.fold_in(jax.random.fold_in(rng, 6), dim), (shards_of,), jnp.float32, least / len(shards), largest / len(shards))
        loudness = loudness * jnp.repeat(jnp.exp(steps), dims[dim] // shards_of).reshape((-1,) + (1,) * (len(dims) - 1 - dim))
    return loudness


def assign_block(own_key, own, number, rows, amount, top, reach, skew):
    ranking = jax.random.permutation(own_key, amount)
    crowded, ordinary = load_shares(amount, rows * top, reach, skew, True), load_shares(amount, rows * top, reach, skew, False)
    places = jnp.arange(amount)

    def named(sizes, turn):
        used = int((sizes > 0).sum())
        fixed = max(1, used // 4)
        passed = fixed + (places - fixed + turn * (used - fixed)) % max(1, amount - fixed)
        return jnp.zeros((amount,), jnp.int32).at[ranking[jnp.where(places < fixed, places, passed)]].set(jnp.asarray(sizes, jnp.int32))

    sizes = jnp.where(number % 4 == 0, named(crowded, number // 4), named(ordinary, number - number // 4 - 1))
    mixed = jax.random.permutation(jax.random.fold_in(own, 3), amount)
    giver, receiver = mixed[0:amount // 2 * 2:2], mixed[1:amount // 2 * 2:2]
    slack = jnp.minimum(sizes[giver] - 1, reach - sizes[receiver]) // 2
    slack = jnp.where((giver == ranking[0]) | (receiver == ranking[0]) | (sizes[receiver] == 0), 0, jnp.maximum(slack, 0))
    passed = jax.random.randint(jax.random.fold_in(own, 4), (amount // 2,), 0, 1 << 20) % (slack + 1)
    sizes = sizes.at[giver].add(-passed).at[receiver].add(passed)
    members = jnp.searchsorted(jnp.cumsum(sizes), jnp.arange(rows * top), side="right").astype(jnp.int32)
    grid = members.reshape(top, rows).T
    grid = grid[jax.random.permutation(jax.random.fold_in(own, 1), rows)]
    turn = jax.random.randint(jax.random.fold_in(own, 2), (rows, 1), 0, top)
    return jnp.take_along_axis(grid, (jnp.arange(top)[None, :] + turn) % top, axis=1)


def load_shares(amount, total, reach, lean, full):
    weights = [(1 << 20) // math.isqrt(grade ** lean) + 1 for grade in range(1, amount + 1)]
    largest = reach if full else min(reach, max(-(-total // amount), total * weights[0] // sum(weights)))
    least = 1 if total - largest >= amount - 1 else 0
    given, surplus = [largest] + [least] * (amount - 1), total - largest - least * (amount - 1)
    while surplus > 0:
        movable = [i for i in range(1, amount) if given[i] < largest] or [i for i in range(1, amount) if given[i] < reach]
        mass, budget = sum([weights[i] for i in movable]), surplus
        for i in movable:
            extra = min(reach - given[i], max(1, budget * weights[i] // mass), surplus)
            given[i] = given[i] + extra
            surplus = surplus - extra
    return np.array(given)


def gaussian(stream_key, shape, width, limit, shards=(), kind=jnp.bfloat16):
    loudness = levels(stream_key, shape, shards, -0.22, 0.18) if shards else 1.0
    entries = jax.random.normal(stream_key, shape, jnp.float32) * width * loudness
    return jnp.minimum(jnp.maximum(entries, -limit), limit).astype(kind)


def gaussian_with(rng, dims, scale, bound, cuts, heavy, kind=jnp.bfloat16):
    values = scale * jax.random.normal(rng, dims, jnp.float32)
    if cuts:
        values = values * levels(rng, dims, cuts, -0.22, 0.18)
    return jnp.clip(with_spikes(values, jax.random.fold_in(rng, 3), *heavy), -bound, bound).astype(kind)


def setup_inputs(seed: int = 0) -> dict:
    splits = jax.random.split(jax.random.key(seed), 13)
    d_out = gaussian_with(splits[0], (SEQUENCE_TOKENS, D), 1.0, 6.0, ((0, 32),), (0, 1, 32, 2.75))
    route_expert_keys = jax.random.split(jax.random.fold_in(splits[1], 1), SEQUENCE_TOKENS // TOK_DEV)
    route_expert_turns = jax.random.permutation(jax.random.fold_in(splits[1], 3), SEQUENCE_TOKENS // TOK_DEV)
    route_expert = jax.vmap(lambda own, number: assign_block(jax.random.fold_in(splits[1], 2), own, number, TOK_DEV, EXPERTS, 2, CAP, 0))(route_expert_keys, route_expert_turns).reshape((SEQUENCE_TOKENS, 2))
    route_weight = jnp.clip(0.2 + 0.8 * jax.random.uniform(splits[2], (SEQUENCE_TOKENS, 2), jnp.float32) ** levels(splits[2], (SEQUENCE_TOKENS, 2), ((0, 32),), -0.2, 0.2), 0.2, 1.0)
    expert_inputs = gaussian(splits[3], (EXPERTS, EXPERTS * CAP, D), 1.0, 6.0, ((0, 32),))
    w_gate = gaussian(splits[4], (EXPERTS, D, FF), D ** -0.5, 0.125, ((0, 32), (2, 4)))
    w_up = gaussian(splits[5], (EXPERTS, D, FF), D ** -0.5, 0.125, ((0, 32), (2, 4)))
    w_down = gaussian(splits[6], (EXPERTS, FF, D), FF ** -0.5, 0.109375, ((0, 32), (1, 4)))
    w_out = gaussian(splits[7], (D, MIXER_HEADS * DV), (MIXER_HEADS * DV) ** -0.5, 0.1875, ((1, 4),))
    queries = gaussian(splits[8], (SEQUENCE_TOKENS, MIXER_HEADS, KEY_CHANNELS), 1.0, 6.0, ((0, 32), (1, 4)))
    keys = gaussian(splits[9], (SEQUENCE_TOKENS, MIXER_HEADS, KEY_CHANNELS), (SEQUENCE_TOKENS ** -0.25), 1.25, ((0, 32), (1, 4)))
    values = gaussian(splits[10], (SEQUENCE_TOKENS, MIXER_HEADS, DV), 1.0, 6.0, ((0, 32), (1, 4)))
    log_decay = draw_log_decay(jax.random.fold_in(splits[12], 71), 0)
    return dict(d_out=d_out, route_expert=route_expert, route_weight=route_weight, expert_inputs=expert_inputs, w_gate=w_gate, w_up=w_up, w_down=w_down, w_out=w_out, queries=queries, keys=keys, values=values, log_decay=log_decay)


precise = lax.Precision.HIGHEST

def block_mixer(scaled_queries, keys_in, values_in, decay_in, initial):
    length, head_count, _ = scaled_queries.shape
    value_width = values_in.shape[-1]
    count_blocks = length // BLK

    def to_blocks(tensor):
        return tensor.reshape(count_blocks, BLK, head_count, tensor.shape[-1]).transpose(0, 2, 1, 3)
    causal = jnp.tril(jnp.ones((BLK, BLK), dtype=bool))[:, :, None]

    def advance(carry_state, inputs):
        query_block, key_block, value_block, decay_block = inputs
        cumulative = jnp.cumsum(decay_block, axis=1)
        ending = cumulative[:, -1, :]
        carried = jnp.einsum('hcd,hde->hce', query_block * jnp.exp(cumulative), carry_state, precision=precise)
        within = jnp.where(causal, jnp.exp(cumulative[:, :, None, :] - cumulative[:, None, :, :]), 0.0)
        scores = jnp.einsum('hid,hjd,hijd->hij', query_block, key_block, within, precision=precise)
        inner_part = jnp.einsum('hij,hje->hie', scores, value_block, precision=precise)
        faded_keys = key_block * jnp.exp(ending[:, None, :] - cumulative)
        carry_state = carry_state * jnp.exp(ending)[:, :, None] + jnp.einsum('hcd,hce->hde', faded_keys, value_block, precision=precise)
        return (carry_state, carried + inner_part)
    final_state, blocks_out = lax.scan(jax.checkpoint(advance), initial, (to_blocks(scaled_queries), to_blocks(keys_in), to_blocks(values_in), to_blocks(decay_in)))
    return (blocks_out.transpose(0, 2, 1, 3).reshape(length, head_count, value_width), final_state)

def expert_pass(rows_in, routed_rows, gate_w, up_w, down_w):
    gate_pre = jnp.dot(rows_in, gate_w, preferred_element_type=jnp.float32)
    up_pre = jnp.dot(rows_in, up_w, preferred_element_type=jnp.float32)
    sigmoid_gate = jax.nn.sigmoid(gate_pre)
    active = gate_pre * sigmoid_gate
    hidden = (active * up_pre).astype(jnp.bfloat16)
    d_hidden = lax.dot_general(routed_rows, down_w, (((1,), (1,)), ((), ())), preferred_element_type=jnp.float32)
    d_gate = (d_hidden * up_pre * sigmoid_gate * (1.0 + gate_pre * (1.0 - sigmoid_gate))).astype(jnp.bfloat16)
    d_up = (d_hidden * active).astype(jnp.bfloat16)
    rows_first = (((0,), (0,)), ((), ()))
    grad_gate = lax.dot_general(rows_in, d_gate, rows_first, preferred_element_type=jnp.float32).astype(jnp.bfloat16)
    grad_up = lax.dot_general(rows_in, d_up, rows_first, preferred_element_type=jnp.float32).astype(jnp.bfloat16)
    grad_down = lax.dot_general(hidden, routed_rows, rows_first, preferred_element_type=jnp.float32).astype(jnp.bfloat16)
    return (grad_gate, grad_up, grad_down, d_gate, d_up)

def reference(d_out, route_expert, route_weight, expert_inputs, w_gate, w_up, w_down, w_out, queries, keys, values, log_decay):
    per_block = route_expert.reshape(N_SP, 2 * TOK_DEV).astype(jnp.int32)
    onehot = (per_block[:, :, None] == jnp.arange(EXPERTS, dtype=jnp.int32)[None, None, :]).astype(jnp.int32)
    before = jnp.cumsum(onehot, axis=1) - onehot
    rank_slot = lax.optimization_barrier(jnp.sum(before * onehot, axis=2))
    source_dev = jnp.arange(N_SP, dtype=jnp.int32)[:, None]
    slot_index = (per_block * (N_SP * CAP) + source_dev * CAP + rank_slot).reshape(-1).astype(jnp.int32)
    scaled = (jnp.repeat(d_out, 2, axis=0).astype(jnp.float32) * route_weight.reshape(-1)[:, None]).astype(jnp.bfloat16)
    routed = jnp.zeros((EXPERTS * N_SP * CAP, D), jnp.bfloat16).at[slot_index].set(scaled).reshape(EXPERTS, N_SP * CAP, D)
    part_width = FF // N_TP

    def one_expert(operands):
        rows_in, routed_rows, gate_w, up_w, down_w = operands
        grad_gate, grad_up, grad_down, d_gate, d_up = expert_pass(rows_in, routed_rows, gate_w, up_w, down_w)
        total = jnp.zeros((rows_in.shape[0], D), jnp.float32)
        for piece in range(N_TP):
            lower = piece * part_width
            term = lax.dot_general(d_gate[:, lower:lower + part_width], gate_w[:, lower:lower + part_width], (((1,), (1,)), ((), ())), preferred_element_type=jnp.float32)
            term = term + lax.dot_general(d_up[:, lower:lower + part_width], up_w[:, lower:lower + part_width], (((1,), (1,)), ((), ())), preferred_element_type=jnp.float32)
            total = total + lax.optimization_barrier(term.astype(jnp.bfloat16)).astype(jnp.float32)
        return (grad_gate, grad_up, grad_down, total.astype(jnp.bfloat16))
    grad_gate, grad_up, grad_down, row_grads = lax.map(one_expert, (expert_inputs, routed, w_gate, w_up, w_down))
    picked = row_grads.reshape(-1, D)[slot_index].astype(jnp.float32).reshape(SEQUENCE_TOKENS, 2, D).sum(axis=1)
    mix_grad = (d_out.astype(jnp.float32) + picked).astype(jnp.bfloat16)
    scale_q = KEY_CHANNELS ** (-0.5)
    initial = jnp.zeros((MIXER_HEADS, KEY_CHANNELS, DV), jnp.float32)

    def mixer_map(query_x, key_x, value_x, decay_x):
        return block_mixer(query_x * scale_q, key_x, value_x, decay_x, initial)[0]
    mixer_out, pullback = jax.vjp(mixer_map, queries.astype(jnp.float32), keys.astype(jnp.float32), values.astype(jnp.float32), log_decay)
    mixed = mixer_out.reshape(SEQUENCE_TOKENS, MIXER_HEADS * DV).astype(jnp.bfloat16)
    grad_proj = lax.dot_general(mix_grad, mixed, (((0,), (0,)), ((), ())), preferred_element_type=jnp.float32)
    d_mixed = jnp.dot(mix_grad, w_out, preferred_element_type=jnp.float32).reshape(SEQUENCE_TOKENS, MIXER_HEADS, DV)
    grad_q, grad_k, grad_v, grad_g = pullback(d_mixed)
    return (grad_gate, grad_up, grad_down, grad_proj, grad_q.astype(jnp.bfloat16), grad_k.astype(jnp.bfloat16), grad_v.astype(jnp.bfloat16), grad_g)
```

```python
import functools

import jax
import jax.numpy as jnp
from jax import lax
from jax.experimental import pallas as pl
from jax.experimental.pallas import tpu as pltpu
from jax.sharding import Mesh
from jax.sharding import PartitionSpec as P

BLK = 64
SP = ("sp_0", "sp_1", "sp_2")
MESH = pl.DeviceIdType.MESH
f32 = jnp.float32
bf16 = jnp.bfloat16
VMEM_SPEC = pl.BlockSpec(memory_space=pltpu.VMEM)
LIMIT = 60 * 1024 * 1024


def mm(a, b, ca, cb):
    return lax.dot_general(
        a.astype(bf16), b.astype(bf16), (((ca,), (cb,)), ((), ())), preferred_element_type=f32
    )


def mm_high(a, b, ca, cb):
    return lax.dot_general(
        a,
        b,
        (((ca,), (cb,)), ((), ())),
        precision=lax.Precision.HIGHEST,
        preferred_element_type=f32,
    )


def call(body, outs, cost, name, **params):
    return pl.pallas_call(
        body,
        out_shape=outs,
        in_specs=params.pop("in_specs"),
        out_specs=jax.tree.map(lambda _: VMEM_SPEC, outs),
        scratch_shapes=params.pop("scratch", []),
        compiler_params=pltpu.CompilerParams(vmem_limit_bytes=LIMIT, **params),
        cost_estimate=pl.CostEstimate(flops=cost, bytes_accessed=1 << 20, transcendentals=0),
        name=name,
    )


def route_body(capacity, expert_ref, weight_ref, d_out_ref, out_ref, slot_ref):
    tok = d_out_ref.shape[0]
    slots = out_ref.shape[0]
    experts = slots // capacity
    e0, e1 = expert_ref[0:1, :], expert_ref[1:2, :]
    w0, w1 = weight_ref[0:1, :], weight_ref[1:2, :]
    eid = lax.broadcasted_iota(jnp.int32, (experts, tok), 0)
    o0, o1 = eid == e0, eid == e1
    named = jnp.where(o0 | o1, 1.0, 0.0).astype(bf16)
    earlier = jnp.where(
        lax.broadcasted_iota(jnp.int32, (tok, tok), 0)
        < lax.broadcasted_iota(jnp.int32, (tok, tok), 1),
        1.0,
        0.0,
    ).astype(bf16)
    count = mm(named, earlier, 1, 0)
    r0 = jnp.sum(jnp.where(o0, count, 0.0), axis=0, keepdims=True)
    r1 = jnp.sum(jnp.where(o1, count, 0.0), axis=0, keepdims=True)
    s0 = e0 * capacity + r0.astype(jnp.int32)
    s1 = e1 * capacity + r1.astype(jnp.int32)
    slot_ref[0:1, :] = s0
    slot_ref[1:2, :] = s1
    step = 128

    def rows(i, _):
        base = pl.multiple_of(i * step, step)
        sid = lax.broadcasted_iota(jnp.int32, (step, tok), 0) + base
        p0, p1 = sid == s0, sid == s1
        pick = jnp.where(p0 | p1, 1.0, 0.0).astype(bf16)
        weight = jnp.sum(
            jnp.where(p0, w0, 0.0) + jnp.where(p1, w1, 0.0), axis=1, keepdims=True
        )
        picked = jnp.dot(pick, d_out_ref[...], preferred_element_type=f32)
        out_ref[pl.ds(base, step), :] = (picked * weight).astype(bf16)
        return 0

    lax.fori_loop(0, slots // step, rows, 0)


def route(expert_t, weight_t, d_out, capacity, experts):
    outs = (
        jax.ShapeDtypeStruct((experts * capacity, d_out.shape[1]), bf16),
        jax.ShapeDtypeStruct(expert_t.shape, jnp.int32),
    )
    return call(
        functools.partial(route_body, capacity), outs, 3 * 10**9, "route", in_specs=[VMEM_SPEC] * 3
    )(expert_t, weight_t, d_out)


def combine_body(slot_ref, returned_ref, own_ref, out_ref):
    tok = own_ref.shape[0]
    slots = returned_ref.shape[0]
    sid = lax.broadcasted_iota(jnp.int32, (tok, slots), 1)
    pick = (sid == slot_ref[:, 0:1]) | (sid == slot_ref[:, 1:2])
    picked = jnp.dot(
        jnp.where(pick, 1.0, 0.0).astype(bf16), returned_ref[...], preferred_element_type=f32
    )
    out_ref[...] = (own_ref[...].astype(f32) + picked).astype(bf16)


def combine(slot_cols, returned, own):
    outs = jax.ShapeDtypeStruct(own.shape, bf16)
    return call(combine_body, outs, 10**9, "combine", in_specs=[VMEM_SPEC] * 3)(
        slot_cols, returned, own
    )


def lower(n):
    return lax.broadcasted_iota(jnp.int32, (n, n), 0) >= lax.broadcasted_iota(
        jnp.int32, (n, n), 1
    )


def produce_body(k_ref, v_ref, g_ref, state_ref, decay_ref, cum_ref):
    tri = jnp.where(lower(BLK), 1.0, 0.0)
    run = jnp.zeros((1, g_ref.shape[1]), f32)
    for c in range(g_ref.shape[0] // BLK):
        rows = pl.ds(c * BLK, BLK)
        b = mm_high(tri, g_ref[rows, :], 1, 0)
        cum_ref[rows, :] = b + run
        run = run + b[BLK - 1 : BLK, :]
    faded = k_ref[...].astype(f32) * jnp.exp(run - cum_ref[...])
    state_ref[...] = mm(v_ref[...], faded, 0, 0)
    decay_ref[...] = jnp.broadcast_to(jnp.exp(run), decay_ref.shape)


def produce(k, v, g):
    outs = (
        jax.ShapeDtypeStruct((v.shape[1], k.shape[1]), f32),
        jax.ShapeDtypeStruct((8, k.shape[1]), f32),
        jax.ShapeDtypeStruct(g.shape, f32),
    )
    return call(produce_body, outs, 10**8, "produce", in_specs=[VMEM_SPEC] * 3)(k, v, g)


def chunk(q_ref, k_ref, g_ref, rows, scale, tri):
    b = mm_high(tri, g_ref[rows, :], 1, 0)
    last = b[BLK - 1 : BLK, :]
    mid = b[BLK // 2 - 1 : BLK // 2, :]
    return b, last, mid, q_ref[rows, :].astype(f32) * scale, k_ref[rows, :].astype(f32)


def forward_body(scale, q_ref, k_ref, v_ref, g_ref, start_ref, mixed_ref, states_ref):
    keep = lower(BLK)
    tri = jnp.where(keep, 1.0, 0.0)
    state = start_ref[...]
    for c in range(g_ref.shape[0] // BLK):
        rows = pl.ds(c * BLK, BLK)
        b, last, mid, q, k = chunk(q_ref, k_ref, g_ref, rows, scale, tri)
        v = v_ref[rows, :]
        states_ref[c] = state
        scores = jnp.where(keep, mm(q * jnp.exp(b - mid), k * jnp.exp(mid - b), 1, 1), 0.0)
        out = mm(q * jnp.exp(b), state, 1, 1) + mm(scores, v, 1, 0)
        mixed_ref[rows, :] = out.astype(bf16)
        state = state * jnp.exp(last) + mm(v, k * jnp.exp(last - b), 0, 0)


def forward(q, k, v, g, start, scale):
    blocks = g.shape[0] // BLK
    outs = (
        jax.ShapeDtypeStruct(v.shape, bf16),
        jax.ShapeDtypeStruct((blocks, *start.shape), f32),
    )
    return call(
        functools.partial(forward_body, scale), outs, 10**9, "forward", in_specs=[VMEM_SPEC] * 5
    )(q, k, v, g, start)


def own_term_body(scale, q_ref, cum_ref, d_ref, out_ref):
    q = q_ref[...].astype(f32) * scale * jnp.exp(cum_ref[...])
    out_ref[...] = mm(d_ref[...], q, 0, 0)


def own_term(q, cum, d_mixed, scale):
    outs = jax.ShapeDtypeStruct((d_mixed.shape[1], q.shape[1]), f32)
    return call(
        functools.partial(own_term_body, scale), outs, 10**8, "own_term", in_specs=[VMEM_SPEC] * 3
    )(q, cum, d_mixed)


def backward_body(
    scale, q_ref, k_ref, v_ref, g_ref, d_ref, states_ref, later_ref, dq_ref, dk_ref, dv_ref, dg_ref
):
    keep = lower(BLK)
    tri = jnp.where(keep, 1.0, 0.0)
    later = later_ref[...]
    for c in reversed(range(g_ref.shape[0] // BLK)):
        rows = pl.ds(c * BLK, BLK)
        b, last, mid, q, k = chunk(q_ref, k_ref, g_ref, rows, scale, tri)
        v = v_ref[rows, :]
        d = d_ref[rows, :]
        state = states_ref[c]
        up, down = jnp.exp(b - mid), jnp.exp(mid - b)
        qt, kt = q * up, k * down
        q_in = q * jnp.exp(b)
        fade = jnp.exp(last - b)
        gone = jnp.exp(last)
        scores = jnp.where(keep, mm(qt, kt, 1, 1), 0.0)
        d_scores = jnp.where(keep, mm(d, v, 1, 1), 0.0)
        dq = up * mm(d_scores, kt, 1, 0) + jnp.exp(b) * mm(d, state, 1, 0)
        k_later = fade * mm(v, later, 1, 0)
        dk = down * mm(d_scores, qt, 0, 0) + k_later
        dv = mm(scores, d, 0, 0) + mm(k * fade, later, 1, 1)
        ends = gone * jnp.sum(state * later, axis=0, keepdims=True) + jnp.sum(
            k * k_later, axis=0, keepdims=True
        )
        dg_ref[rows, :] = mm_high(tri, q * dq - k * dk, 0, 0) + ends
        dq_ref[rows, :] = (dq * scale).astype(bf16)
        dk_ref[rows, :] = dk.astype(bf16)
        dv_ref[rows, :] = dv.astype(bf16)
        later = later * gone + mm(d, q_in, 0, 0)


def backward(q, k, v, g, d_mixed, states, later, scale):
    outs = (
        jax.ShapeDtypeStruct(q.shape, bf16),
        jax.ShapeDtypeStruct(k.shape, bf16),
        jax.ShapeDtypeStruct(v.shape, bf16),
        jax.ShapeDtypeStruct(g.shape, f32),
    )
    return call(
        functools.partial(backward_body, scale), outs, 2 * 10**9, "backward", in_specs=[VMEM_SPEC] * 7
    )(q, k, v, g, d_mixed, states, later)


def scan_level(own_state, own_decay, axis, reverse, bufs, sems):
    state_buf, decay_buf = bufs
    send_s, recv_s, send_d, recv_d = sems
    n = lax.axis_size(axis)
    me = lax.axis_index(axis)
    state_buf[0] = own_state.astype(bf16)
    decay_buf[0] = own_decay
    copies = []
    for shift in range(1, n):
        peer = lax.rem(me + shift, n)
        for buf, send, recv in ((state_buf, send_s, recv_s), (decay_buf, send_d, recv_d)):
            copy = pltpu.make_async_remote_copy(
                src_ref=buf.at[0],
                dst_ref=buf.at[shift],
                send_sem=send.at[shift],
                recv_sem=recv.at[shift],
                device_id={axis: peer},
                device_id_type=MESH,
            )
            copy.start()
            copies.append(copy)
    for copy in copies:
        copy.wait()
    before = jnp.zeros_like(own_state)
    total = jnp.zeros_like(own_state)
    before_decay = jnp.ones_like(own_decay)
    total_decay = jnp.ones_like(own_decay)
    for k in reversed(range(n)) if reverse else range(n):
        place = lax.rem(me - k + n, n)
        state = jnp.where(place == 0, own_state, state_buf[place].astype(f32))
        decay = decay_buf[place]
        total = total * decay[0:1, :] + state
        total_decay = total_decay * decay
        passed = k > me if reverse else k < me
        before = jnp.where(passed, total, before)
        before_decay = jnp.where(passed, total_decay, before_decay)
    return before, before_decay, total, total_decay


def exchange_body(reverse, axes, state_ref, decay_ref, out_ref, *scratch):
    barrier = pltpu.get_barrier_semaphore()
    peers = 0
    for axis in axes:
        n = lax.axis_size(axis)
        for shift in range(1, n):
            peer = lax.rem(lax.axis_index(axis) + shift, n)
            pl.semaphore_signal(barrier, inc=1, device_id={axis: peer}, device_id_type=MESH)
            peers += 1
    pl.semaphore_wait(barrier, peers)
    total, total_decay = state_ref[...], decay_ref[...]
    before = jnp.zeros_like(total)
    for level, axis in enumerate(reversed(axes)):
        part = scratch[6 * level : 6 * level + 6]
        inside, inside_decay, total, total_decay = scan_level(
            total, total_decay, axis, reverse, part[:2], part[2:]
        )
        if level == 0:
            before, before_decay = inside, inside_decay
        else:
            before = before_decay[0:1, :] * inside + before
            before_decay = before_decay * inside_decay
    out_ref[...] = before


def exchange(state, decay, axes, reverse, collective_id):
    scratch = []
    for axis in reversed(axes):
        n = lax.axis_size(axis)
        scratch += [pltpu.VMEM((n, *state.shape), bf16), pltpu.VMEM((n, *decay.shape), f32)]
        scratch += [pltpu.SemaphoreType.DMA((n,))] * 4
    return call(
        functools.partial(exchange_body, reverse, axes),
        jax.ShapeDtypeStruct(state.shape, f32),
        10**8,
        "exchange_reverse" if reverse else "exchange_forward",
        in_specs=[VMEM_SPEC] * 2,
        scratch=scratch,
        collective_id=collective_id,
        has_side_effects=True,
    )(state, decay)


def split_up(x, dim, count):
    before, after = (x.shape[:dim], x.shape[dim + 1 :])
    return jnp.moveaxis(x.reshape(*before, count, -1, *after), dim, 0)


def summed_on_arrival(x, axis, dim):
    count = lax.axis_size(axis)
    tiles = lax.all_to_all(split_up(x, dim, count), axis, 0, 0, tiled=True)
    return jnp.sum(tiles.astype(f32), axis=0)


def joined_along(tiles, dim):
    dims = list(tiles.shape[1:])
    dims[dim] *= tiles.shape[0]
    return jnp.moveaxis(tiles, 0, dim).reshape(dims)


def gathered_copies(x, axis, dim):
    count = lax.axis_size(axis)
    sent = lax.all_to_all(jnp.broadcast_to(x[None], (count, *x.shape)), axis, 0, 0, tiled=True)
    return joined_along(sent, dim)


def expert_pass(rows_in, routed_rows, gate_w, up_w, down_w):
    gate_pre = jnp.dot(rows_in, gate_w, preferred_element_type=f32)
    up_pre = jnp.dot(rows_in, up_w, preferred_element_type=f32)
    sigmoid_gate = jax.nn.sigmoid(gate_pre)
    active = gate_pre * sigmoid_gate
    hidden = (active * up_pre).astype(bf16)
    d_hidden = lax.dot_general(
        routed_rows, down_w, (((1,), (1,)), ((), ())), preferred_element_type=f32
    )
    d_gate = (d_hidden * up_pre * sigmoid_gate * (1.0 + gate_pre * (1.0 - sigmoid_gate))).astype(
        bf16
    )
    d_up = (d_hidden * active).astype(bf16)
    rows_first = (((0,), (0,)), ((), ()))
    grad_gate = lax.dot_general(rows_in, d_gate, rows_first, preferred_element_type=f32).astype(
        bf16
    )
    grad_up = lax.dot_general(rows_in, d_up, rows_first, preferred_element_type=f32).astype(bf16)
    grad_down = lax.dot_general(
        hidden, routed_rows, rows_first, preferred_element_type=f32
    ).astype(bf16)
    return (grad_gate, grad_up, grad_down, d_gate, d_up)


def local(
    d_out,
    route_expert,
    route_weight,
    expert_inputs,
    w_gate,
    w_up,
    w_down,
    w_out,
    queries,
    keys,
    values,
    log_decay,
):
    tok_rows, model_width = d_out.shape
    experts = lax.axis_size(SP)
    capacity = expert_inputs.shape[1] // experts
    quarter = model_width // lax.axis_size("tp")
    own_cols = lax.dynamic_slice_in_dim(d_out, lax.axis_index("tp") * quarter, quarter, 1)
    outbox, slots = route(route_expert.T, route_weight.T, d_out, capacity, experts)
    routed = lax.all_to_all(
        outbox.reshape(experts, capacity, model_width), SP, split_axis=0, concat_axis=0, tiled=True
    ).reshape(experts * capacity, model_width)

    scale = queries.shape[2] ** (-0.5)
    q, k, v, g = (x.reshape(tok_rows, x.shape[2]) for x in (queries, keys, values, log_decay))
    produced, decay, cum = produce(k, v, g)
    start = exchange(produced, decay, SP, False, 0)
    mixed, states = forward(q, k, v, g, start, scale)

    gate_w, up_w = w_gate[0], w_up[0]
    grad_gate, grad_up, grad_down, d_gate, d_up = expert_pass(
        expert_inputs[0], routed, gate_w, up_w, w_down[0]
    )
    cols = (((1,), (1,)), ((), ()))
    partial_terms = lax.dot_general(d_gate, gate_w, cols, preferred_element_type=f32)
    partial_terms = partial_terms + lax.dot_general(d_up, up_w, cols, preferred_element_type=f32)
    summed = summed_on_arrival(partial_terms.astype(bf16), "tp", 1)
    returned = lax.all_to_all(
        summed.astype(bf16).reshape(experts, capacity, quarter),
        SP,
        split_axis=0,
        concat_axis=0,
        tiled=True,
    ).reshape(experts * capacity, quarter)
    mix_cols = combine(slots.T, returned, own_cols)
    mix_grad = gathered_copies(mix_cols, "tp", 1)
    grad_proj = lax.psum_scatter(
        lax.dot_general(
            mix_grad, mixed, (((0,), (0,)), ((), ())), preferred_element_type=f32
        ).astype(bf16),
        SP,
        scatter_dimension=0,
        tiled=True,
    ).astype(f32)
    d_mixed = jnp.dot(mix_grad, w_out, preferred_element_type=f32)
    later = exchange(own_term(q, cum, d_mixed, scale), decay, SP, True, 1)
    grad_q, grad_k, grad_v, grad_g = backward(q, k, v, g, d_mixed, states, later, scale)
    return (
        grad_gate[None],
        grad_up[None],
        grad_down[None],
        grad_proj,
        grad_q.reshape(queries.shape),
        grad_k.reshape(keys.shape),
        grad_v.reshape(values.shape),
        grad_g.reshape(log_decay.shape),
    )


def solution(mesh):
    finer = Mesh(mesh.devices.reshape(4, 4, 2, mesh.shape["tp"]), (*SP, "tp"))
    return jax.shard_map(
        local,
        mesh=finer,
        in_specs=(
            P(SP, None),
            P(SP, None),
            P(SP, None),
            P(SP, None, None),
            P(SP, None, "tp"),
            P(SP, None, "tp"),
            P(SP, "tp", None),
            P(None, "tp"),
            P(SP, "tp", None),
            P(SP, "tp", None),
            P(SP, "tp", None),
            P(SP, "tp", None),
        ),
        out_specs=(
            P(SP, None, "tp"),
            P(SP, None, "tp"),
            P(SP, "tp", None),
            P(SP, "tp"),
            P(SP, "tp", None),
            P(SP, "tp", None),
            P(SP, "tp", None),
            P(SP, "tp", None),
        ),
        check_vma=False,
    )
```
